32 devices in a mesh: sp: 8 (over z, x), tp: 4 (over y, core).
Axes of the slice: x: 2, y: 2, z: 4, core: 2. Of those that a mesh axis runs over, the one named last changes fastest.
Arguments:
- tokens: bfloat16 [1024, 1024], P('sp', 'tp'), may hold values from -6 to 6
- norm_gain: float32 [3, 1024], replicated, may hold values from 0.1 to 1.9
- w_query: bfloat16 [3, 1024, 1024], P(None, 'sp', 'tp'), may hold values from -0.1875 to 0.1875
- w_key: bfloat16 [3, 1024, 1024], P(None, 'sp', 'tp'), may hold values from -0.1875 to 0.1875
- w_value: bfloat16 [3, 1024, 1024], P(None, 'sp', 'tp'), may hold values from -0.1875 to 0.1875
- w_out: bfloat16 [3, 1024, 1024], P(None, 'tp', 'sp'), may hold values from -0.5625 to 0.5625
- offset_bias: float32 [3, 16, 8, 16], P(None, 'tp'), may hold values from -3 to 3
- documents: int32 [1024], P('sp'), may hold values from 0 to 7, never falling along the last dimension, each value on 1 to 256 neighbouring positions
Outputs:
- mixed: bfloat16 [1024, 1024], P('sp', 'tp')
The draws below stay inside these ranges and needn't reach their ends.
Inputs may be any that keep to these rules, and one draw needn't show every extreme that they name: `documents`: document numbers never fall along the token order, start at 0, and each document has 1 to 256 tokens.
All inputs are finite; a program needn't handle non-finite values.
Results may differ from the reference program's by a relative error of at most 0.02.
Values may be sent and summed in bfloat16 or wider, within the bound.
A program may use at most 64 MiB of HBM per device.

```python
import math
import jax
import jax.numpy as jnp
import numpy as np
from jax import lax

HEADS = 16
HEAD_DIM = 64
D = 1024
WIN_ROWS = 8
WIN_COLS = 16
LAYERS = 3
ROWS_DEV = 4
GRID_W = 32
TOKENS = 1024


def level_of(own_key, dims, pieces, low, largest):
    factor_of = 1.0
    for dim, blocks in pieces:
        heights = jax.random.uniform(jax.random.fold_in(jax.random.fold_in(own_key, 6), dim), (blocks,), jnp.float32, low / len(pieces), largest / len(pieces))
        factor_of = factor_of * jnp.repeat(jnp.exp(heights), dims[dim] // blocks).reshape((-1,) + (1,) * (len(dims) - 1 - dim))
    return factor_of


def length_profile(number_of, total, most, slope):
    weights = [(1 << 20) // math.isqrt(grade ** slope) + 1 for grade in range(2, number_of + 1)]
    spare, given = total - most - (number_of - 1), [1] * (number_of - 1)
    while spare > 0:
        movable = [i for i in range(number_of - 1) if given[i] < most]
        whole, left = sum([weights[i] for i in movable]), spare
        for i in movable:
            more = min(most - given[i], max(1, left * weights[i] // whole), spare)
            given[i] = given[i] + more
            spare = spare - more
    return np.array([most] + given)


def uneven_parts(own_key, count, total, most, skew):
    if count == 2:
        one = jax.random.randint(own_key, (), max(1, total - most), min(most, total - 1) + 1)
        return jnp.stack([one, total - one])
    lengths = jnp.asarray(length_profile(count, total, most, skew), jnp.int32)
    pairs = (count - 1) // 2
    giver, sink = lengths[1:1 + 2 * pairs:2], lengths[2:2 + 2 * pairs:2]
    margin = jnp.minimum(giver - 1, most - sink)
    shifted = jax.random.randint(jax.random.fold_in(own_key, 1), (pairs,), 0, 1 << 20) % (margin + 1)
    lengths = lengths.at[1:1 + 2 * pairs:2].set(giver - shifted).at[2:2 + 2 * pairs:2].set(sink + shifted)
    return lengths[jax.random.permutation(jax.random.fold_in(own_key, 2), count)]


def centred(stream_key, shape, deviation, bound, split=(), held_as=jnp.bfloat16):
    result = deviation * jax.random.normal(stream_key, shape, jnp.float32)
    if split:
        result = result * level_of(stream_key, shape, split, -0.22, 0.18)
    return jnp.clip(result, -bound, bound).astype(held_as)


def setup_inputs(seed: int = 0) -> dict:
    keys = jax.random.split(jax.random.key(seed), 9)
    return {
        "tokens": centred(keys[0], (TOKENS, D), 1.0, 6.0, ((0, 8), (1, 4))),
        "norm_gain": jnp.clip(1.0 + 0.18 * jax.random.normal(keys[1], (LAYERS, D), jnp.float32), 0.1, 1.9),
        "w_query": centred(keys[2], (LAYERS, D, D), D ** -0.5, 0.1875, ((1, 8), (2, 4))),
        "w_key": centred(keys[3], (LAYERS, D, D), D ** -0.5, 0.1875, ((1, 8), (2, 4))),
        "w_value": centred(keys[4], (LAYERS, D, D), D ** -0.5, 0.1875, ((1, 8), (2, 4))),
        "w_out": centred(keys[5], (LAYERS, D, D), (3.0 / D ** 0.5), 0.5625, ((1, 4), (2, 8))),
        "offset_bias": centred(keys[6], (LAYERS, HEADS, WIN_ROWS, WIN_COLS), 0.5, 3.0, ((1, 4),), jnp.float32),
        "documents": jnp.searchsorted(jnp.cumsum(uneven_parts(keys[7], TOKENS // (ROWS_DEV * GRID_W), TOKENS, 2 * ROWS_DEV * GRID_W, 2)), jnp.arange(TOKENS), side="right").astype(jnp.int32),
    }


EPS = 1e-06

def rms_rows(stream, gain_row):
    values = stream.astype(jnp.float32)
    mean_sq = lax.optimization_barrier(jnp.mean(values * values, axis=-1, keepdims=True))
    return (values * lax.rsqrt(mean_sq + EPS) * gain_row).astype(jnp.bfloat16)

def head_norm(heads_raw):
    values = heads_raw.astype(jnp.float32)
    mean_sq = lax.optimization_barrier(jnp.mean(values * values, axis=-1, keepdims=True))
    return (values * lax.rsqrt(mean_sq + EPS)).astype(jnp.bfloat16)

def attend(queries, fringe, seg_own, seg_fringe, bias_layer):
    row_count, grid_width, head_count, head_width = queries.shape
    key_rows = jnp.stack([fringe[row_lag:row_lag + row_count] for row_lag in range(WIN_ROWS)], axis=1)
    seg_rows = jnp.stack([seg_fringe[row_lag:row_lag + row_count] for row_lag in range(WIN_ROWS)], axis=1)
    key_part = key_rows[..., :head_width].astype(jnp.float32)
    value_part = key_rows[..., head_width:].astype(jnp.float32)
    scores = jnp.einsum('rchd,rjkhd->rhcjk', queries.astype(jnp.float32), key_part) * head_width ** (-0.5)
    column = jnp.arange(grid_width)
    col_offset = column[None, :] - column[:, None] + WIN_COLS // 2
    inside = (col_offset >= 0) & (col_offset < WIN_COLS)
    bias_table = bias_layer[:, :, jnp.clip(col_offset, 0, WIN_COLS - 1)]
    scores = scores + jnp.transpose(bias_table, (0, 2, 1, 3))[None]
    same_doc = seg_rows[:, None, None, :, :] == seg_own[:, None, :, None, None]
    allowed = same_doc & inside[None, None, :, None, :]
    scores = jnp.where(allowed, scores, -1e+30)
    flat = scores.reshape(row_count, head_count, grid_width, WIN_ROWS * grid_width)
    attn_probs = jax.nn.softmax(flat, axis=-1).astype(jnp.bfloat16)
    attn_probs = attn_probs.reshape(row_count, head_count, grid_width, WIN_ROWS, grid_width)
    mixed_heads = jnp.einsum('rhcjk,rjkhd->rchd', attn_probs.astype(jnp.float32), value_part)
    return mixed_heads.astype(jnp.bfloat16)

def reference(tokens, norm_gain, w_query, w_key, w_value, w_out, offset_bias, documents):
    row_count = TOKENS // GRID_W
    reach_rows = WIN_ROWS // 2
    seg_own = (documents + 1).reshape(row_count, GRID_W)
    seg_fringe = jnp.pad(seg_own, ((reach_rows, reach_rows), (0, 0)))
    stream = tokens
    for layer_index in range(LAYERS):
        normed = rms_rows(stream, norm_gain[layer_index])
        query_raw = jnp.dot(normed, w_query[layer_index], preferred_element_type=jnp.float32).astype(jnp.bfloat16)
        key_raw = jnp.dot(normed, w_key[layer_index], preferred_element_type=jnp.float32).astype(jnp.bfloat16)
        value_heads = jnp.dot(normed, w_value[layer_index], preferred_element_type=jnp.float32).astype(jnp.bfloat16)
        query_heads = head_norm(query_raw.reshape(row_count, GRID_W, HEADS, HEAD_DIM))
        key_heads = head_norm(key_raw.reshape(row_count, GRID_W, HEADS, HEAD_DIM))
        value_heads = value_heads.reshape(row_count, GRID_W, HEADS, HEAD_DIM)
        key_value = jnp.concatenate([key_heads, value_heads], axis=-1)
        fringe = jnp.pad(key_value, ((reach_rows, reach_rows), (0, 0), (0, 0), (0, 0)))
        attended = attend(query_heads, fringe, seg_own, seg_fringe, offset_bias[layer_index])
        attended = attended.reshape(TOKENS, HEADS * HEAD_DIM)
        stream = jnp.dot(attended, w_out[layer_index], preferred_element_type=jnp.float32).astype(jnp.bfloat16)
    return stream
```

```python
import functools

import jax
import jax.numpy as jnp
from jax import lax
from jax.experimental import pallas as pl
from jax.experimental.pallas import tpu as pltpu
from jax.sharding import PartitionSpec as P

HEAD_DIM = 64
WIN_ROWS = 8
WIN_COLS = 16
GRID_W = 32
EPS = 1e-06
MESH = pl.DeviceIdType.MESH
F32, BF16 = jnp.float32, jnp.bfloat16
K, V, Q, O = 0, 1, 2, 3


def kernel(n, nt, xs, layers, heads, tok_ref, gain_ref, wq_ref, wk_ref, wv_ref, wo_ref, bias_ref, doc_ref,
           out_ref, wbuf, obuf, xg, kv, part, s1, cs, s2, att, strip, dmask, docs,
           own_sem, w_send, w_recv, g_send, g_recv, h_send, h_recv, d_send, d_recv,
           r_send, r_recv, y_send, y_recv, b_send, b_recv):
    me, tp = lax.axis_index("sp"), lax.axis_index("tp")
    zs = n // xs
    toks, feat = tok_ref.shape
    reach = (WIN_ROWS // 2) * GRID_W
    after = reach - GRID_W
    wrows = wq_ref.shape[1]

    def pos_of(sp):
        z, x = sp // xs, sp % xs
        odd = x % 2
        return x * zs + z * (1 - odd) + (zs - 1 - z) * odd

    def sp_of(pos):
        x, z = pos // zs, pos % zs
        odd = x % 2
        return (z * (1 - odd) + (zs - 1 - z) * odd) * xs + x

    pos = pos_of(me)
    right, left = sp_of((pos + 1) % n), sp_of((pos + n - 1) % n)
    core = tp % 2
    mate = tp + 1 - 2 * core
    ymate = (tp + nt // 2) % nt
    has_prev = (me + n - 1) // n
    has_next = 1 - (me + 1) // n

    owns = []
    for l in range(layers):
        for c, ref in ((K, wk_ref), (V, wv_ref), (Q, wq_ref), (O, wo_ref)):
            dst = obuf.at[l, me] if c == O else wbuf.at[l, c, pl.ds(me * wrows, wrows)]
            copy = pltpu.make_async_copy(ref.at[l], dst, own_sem.at[l, c])
            copy.start()
            owns.append(copy)

    barrier = pltpu.get_barrier_semaphore()
    for peer in (left, right):
        pl.semaphore_signal(barrier, inc=1, device_id=(peer, tp), device_id_type=MESH)
    for d in range(1, nt):
        pl.semaphore_signal(barrier, inc=1, device_id=(me, (tp + d) % nt), device_id_type=MESH)

    @pl.when(me > 0)
    def _():
        pl.semaphore_signal(barrier, inc=1, device_id=(me - 1, tp), device_id_type=MESH)

    @pl.when(me < n - 1)
    def _():
        pl.semaphore_signal(barrier, inc=1, device_id=(me + 1, tp), device_id_type=MESH)

    pl.semaphore_wait(barrier, 1 + nt + has_prev + has_next)

    pending = []

    def remote(src, dst, send, recv, device):
        return pltpu.make_async_remote_copy(src_ref=src, dst_ref=dst, send_sem=send, recv_sem=recv,
                                            device_id=device, device_id_type=MESH)

    half = n // 2
    RIGHTLAST, LEFTLAST = (K, V), (Q, O)

    def w_chunks(direction, step):
        if step < half:
            return (K, V, Q, O)
        if step == half:
            return RIGHTLAST if direction == 0 else LEFTLAST
        return ()

    def w_copy(direction, l, step, c):
        if direction == 0:
            origin, peer = sp_of((pos + n - (step - 1)) % n), right
        else:
            origin, peer = sp_of((pos + step - 1) % n), left
        ref = obuf.at[l, origin] if c == O else wbuf.at[l, c, pl.ds(origin * wrows, wrows)]
        return remote(ref, ref, w_send.at[direction, l, step - 1, c], w_recv.at[direction, l, step - 1, c],
                      (peer, tp))

    def w_arrive(direction, l, step, c):
        if direction == 0:
            origin = sp_of((pos + n - step) % n)
        else:
            origin = sp_of((pos + step) % n)
        ref = obuf.at[l, origin] if c == O else wbuf.at[l, c, pl.ds(origin * wrows, wrows)]
        remote(ref, ref, w_send.at[direction, l, step - 1, c], w_recv.at[direction, l, step - 1, c],
               (right if direction == 0 else left, tp)).wait_recv()

    def w_first(l):
        for c in range(4):
            owns[l * 4 + c].wait()
            for direction in range(2):
                if c in w_chunks(direction, 1):
                    copy = w_copy(direction, l, 1, c)
                    copy.start()
                    pending.append(copy)

    def w_step(l, step):
        for c in range(4):
            for direction in range(2):
                if c in w_chunks(direction, step):
                    w_arrive(direction, l, step, c)
                if c in w_chunks(direction, step + 1):
                    copy = w_copy(direction, l, step + 1, c)
                    copy.start()
                    pending.append(copy)

    tasks = []
    for l in range(layers):
        if l:
            tasks.append((l, functools.partial(w_first, l)))
        for step in range(1, half + 1):
            tasks.append((l, functools.partial(w_step, l, step)))

    def work(count, limit):
        while count > 0 and tasks and tasks[0][0] <= limit:
            tasks.pop(0)[1]()
            count -= 1

    w_first(0)
    gathers = []
    for d in range(1, nt):
        copy = remote(tok_ref, xg.at[0, tp], g_send.at[d - 1], g_recv.at[d - 1], (me, (tp + d) % nt))
        copy.start()
        gathers.append(copy)
    xg[0, tp] = tok_ref[...]

    def to_prev(src, dst, k):
        return remote(src, dst, h_send.at[0, k], h_recv.at[0, k], (jnp.maximum(me - 1, 0), tp))

    def to_next(src, dst, k):
        return remote(src, dst, h_send.at[1, k], h_recv.at[1, k], (jnp.minimum(me + 1, n - 1), tp))

    doc_prev = remote(doc_ref, docs.at[2], d_send.at[0], d_recv.at[0], ((me + n - 1) % n, tp))
    doc_next = remote(doc_ref, docs.at[0], d_send.at[1], d_recv.at[1], ((me + 1) % n, tp))

    @pl.when(me > 0)
    def _():
        doc_prev.start()

    @pl.when(me < n - 1)
    def _():
        doc_next.start()

    docs[1] = doc_ref[...]

    @pl.when(me == 0)
    def _():
        docs[0] = jnp.full_like(doc_ref, -1)
        for l in range(layers):
            kv[l, 0:reach] = jnp.zeros((reach, 2 * feat), BF16)

    @pl.when(me == n - 1)
    def _():
        docs[2] = jnp.full_like(doc_ref, -1)
        for l in range(layers):
            kv[l, reach + toks:reach + toks + after] = jnp.zeros((after, 2 * feat), BF16)

    for l in range(layers):
        for h in range(heads):
            row = jnp.broadcast_to(bias_ref[l * heads + h:l * heads + h + 1, :], (GRID_W, WIN_ROWS * GRID_W))
            strip[l, h] = pltpu.roll(row, WIN_ROWS * GRID_W - WIN_COLS // 2, 1, stride=1, stride_axis=0)

    work(1, 0)

    @pl.when(me > 0)
    def _():
        doc_next.wait_recv()

    @pl.when(me < n - 1)
    def _():
        doc_prev.wait_recv()

    seg = [docs[i].astype(F32) for i in range(3)]
    seg_row = jnp.concatenate(seg, axis=1)
    seg_col = jnp.transpose(jnp.broadcast_to(seg[1], (toks, toks)))
    lane = lax.broadcasted_iota(jnp.int32, (GRID_W, WIN_ROWS * GRID_W), 1) % GRID_W
    col = lax.broadcasted_iota(jnp.int32, (GRID_W, WIN_ROWS * GRID_W), 0)
    off = lane - col + WIN_COLS // 2
    inside = (off >= 0) & (off < WIN_COLS)
    rows = toks // GRID_W
    for r in range(rows):
        keys = seg_row[:, r * GRID_W:(r + WIN_ROWS) * GRID_W]
        mine = seg_col[r * GRID_W:(r + 1) * GRID_W, 0:1]
        dmask[r] = jnp.where(inside & (keys == mine), 0.0, -1e30)

    work(1, 0)
    for copy in gathers:
        copy.wait_recv()

    def head_norm(raw, scale):
        raw = raw.astype(BF16).astype(F32)
        sq = raw * raw
        outs = []
        for h in range(heads):
            cut = slice(h * HEAD_DIM, (h + 1) * HEAD_DIM)
            mean = jnp.sum(sq[:, cut], axis=-1, keepdims=True) * (1.0 / HEAD_DIM)
            outs.append(raw[:, cut] * (lax.rsqrt(mean + EPS) * scale))
        return jnp.concatenate(outs, axis=1).astype(BF16)

    for l in range(layers):
        x = [xg[l, q].astype(F32) for q in range(nt)]
        total = sum(jnp.sum(v * v, axis=-1, keepdims=True) for v in x)
        inv = lax.rsqrt(total * (1.0 / (nt * feat)) + EPS)
        normed = jnp.concatenate(
            [(x[q] * inv * gain_ref[l:l + 1, q * feat:(q + 1) * feat]).astype(BF16) for q in range(nt)], axis=1)
        while tasks and tasks[0][0] <= l:
            work(1, l)
        if l + 1 < layers:
            work(1, l + 1)

        own = slice(reach, reach + toks)
        kv[l, own, 0:feat] = head_norm(jnp.dot(normed, wbuf[l, K], preferred_element_type=F32), 1.0)
        kv[l, own, feat:2 * feat] = jnp.dot(normed, wbuf[l, V], preferred_element_type=F32).astype(BF16)
        up = to_next(kv.at[l, own], kv.at[l, 0:reach], l)
        down = to_prev(kv.at[l, reach:reach + after], kv.at[l, reach + toks:reach + toks + after], l)

        @pl.when(me < n - 1)
        def _():
            up.start()

        @pl.when(me > 0)
        def _():
            down.start()

        query = head_norm(jnp.dot(normed, wbuf[l, Q], preferred_element_type=F32), HEAD_DIM ** -0.5)
        work(1, l + 1)

        @pl.when(me > 0)
        def _():
            up.wait_recv()

        @pl.when(me < n - 1)
        def _():
            down.wait_recv()

        for h in range(heads):
            cut = slice(h * HEAD_DIM, (h + 1) * HEAD_DIM)
            for r in range(rows):
                win = slice(r * GRID_W, (r + WIN_ROWS) * GRID_W)
                qr = query[r * GRID_W:(r + 1) * GRID_W, cut]
                s = lax.dot_general(qr, kv[l, win, cut], (((1,), (1,)), ((), ())), preferred_element_type=F32)
                p = jnp.exp(s + strip[l, h] + dmask[r])
                den = jnp.sum(p, axis=-1, keepdims=True)
                vals = kv[l, win, feat + h * HEAD_DIM:feat + (h + 1) * HEAD_DIM]
                o = jnp.dot(p.astype(BF16), vals, preferred_element_type=F32)
                att[r * GRID_W:(r + 1) * GRID_W, cut] = (o / den).astype(BF16)

        work(1, l + 1)
        a = att[...]
        per = feat // wo_ref.shape[2]

        def mix(q):
            return jnp.concatenate(
                [jnp.dot(a, obuf[l, q * per + i], preferred_element_type=F32) for i in range(per)], axis=1)

        s1c = []
        for j in range(2):
            part[l, j] = mix(1 - core + 2 * j).astype(BF16)
            copy = remote(part.at[l, j], s1.at[l, j], r_send.at[l, j], r_recv.at[l, j], (me, mate))
            copy.start()
            s1c.append(copy)
            pending.append(copy)
        mine = [mix(core + 2 * j) for j in range(2)]
        last = l == layers - 1
        if not last:
            s2c = []
            for j in range(2):
                s1c[j].wait_recv()
                cs[l, j] = (mine[j] + s1[l, j].astype(F32)).astype(BF16)
                copy = remote(cs.at[l, j], s2.at[l, j], y_send.at[l, j], y_recv.at[l, j], (me, ymate))
                copy.start()
                s2c.append(copy)
                pending.append(copy)
            work(1, l + 1)
            s3c = []
            for j in range(2):
                s2c[j].wait_recv()
                slot = core + 2 * j
                xg[l + 1, slot] = (cs[l, j].astype(F32) + s2[l, j].astype(F32)).astype(BF16)
                copy = remote(xg.at[l + 1, slot], xg.at[l + 1, slot], b_send.at[l, j], b_recv.at[l, j], (me, mate))
                copy.start()
                s3c.append(copy)
                pending.append(copy)
            for j in range(2):
                s3c[j].wait_recv()
        else:
            y = tp // 2
            for j in range(2):
                s1c[j].wait_recv()
                cs[l, j] = (mine[j] + s1[l, j].astype(F32)).astype(BF16)
            copy = remote(cs.at[l, 1 - y], s2.at[l, 0], y_send.at[l, 0], y_recv.at[l, 0], (me, ymate))
            copy.start()
            pending.append(copy)
            copy.wait_recv()
            out_ref[...] = (cs[l, y].astype(F32) + s2[l, 0].astype(F32)).astype(BF16)

        @pl.when(me < n - 1)
        def _():
            up.wait_send()

        @pl.when(me > 0)
        def _():
            down.wait_send()

    for copy in gathers + pending:
        copy.wait_send()

    @pl.when(me > 0)
    def _():
        doc_prev.wait_send()

    @pl.when(me < n - 1)
    def _():
        doc_next.wait_send()


def solution(mesh):
    n, nt = mesh.shape["sp"], mesh.shape["tp"]
    try:
        xs = len({d.coords[0] for d in mesh.devices.flat})
    except AttributeError:
        xs = 2
    if n % xs or xs % 2:
        xs = 1

    def body(tokens, norm_gain, w_query, w_key, w_value, w_out, offset_bias, documents):
        layers, heads = offset_bias.shape[:2]
        toks, feat = tokens.shape
        model = nt * feat
        bias = jnp.pad(offset_bias, ((0, 0), (0, 0), (0, 0), (0, GRID_W - WIN_COLS)))
        bias = bias.reshape(layers * heads, WIN_ROWS * GRID_W)
        docs = documents.reshape(1, toks)
        reach = (WIN_ROWS // 2) * GRID_W
        dma = lambda *s: pltpu.SemaphoreType.DMA(s)
        vmem, hbm = pl.BlockSpec(memory_space=pltpu.VMEM), pl.BlockSpec(memory_space=pl.ANY)
        blocks = (layers, 2, toks, feat)
        return pl.pallas_call(
            functools.partial(kernel, n, nt, xs, layers, heads),
            out_shape=jax.ShapeDtypeStruct((toks, feat), BF16),
            in_specs=[vmem, vmem, hbm, hbm, hbm, hbm, vmem, vmem],
            out_specs=vmem,
            scratch_shapes=[
                pltpu.VMEM((layers, 3, model, feat), BF16),
                pltpu.VMEM((layers, n, feat, w_out.shape[2]), BF16),
                pltpu.VMEM((layers, nt, toks, feat), BF16),
                pltpu.VMEM((layers, 2 * reach - GRID_W + toks, 2 * feat), BF16),
                pltpu.VMEM(blocks, BF16),
                pltpu.VMEM(blocks, BF16),
                pltpu.VMEM(blocks, BF16),
                pltpu.VMEM(blocks, BF16),
                pltpu.VMEM((toks, feat), BF16),
                pltpu.VMEM((layers, heads, GRID_W, WIN_ROWS * GRID_W), F32),
                pltpu.VMEM((toks // GRID_W, GRID_W, WIN_ROWS * GRID_W), F32),
                pltpu.VMEM((3, 1, toks), jnp.int32),
                dma(layers, 4),
                dma(2, layers, n // 2, 4), dma(2, layers, n // 2, 4),
                dma(nt - 1), dma(nt - 1),
                dma(2, layers), dma(2, layers),
                dma(2), dma(2),
                dma(layers, 2), dma(layers, 2),
                dma(layers, 2), dma(layers, 2),
                dma(layers, 2), dma(layers, 2),
            ],
            compiler_params=pltpu.CompilerParams(
                collective_id=0, has_side_effects=True, vmem_limit_bytes=48 * 1024 * 1024
            ),
        )(tokens, norm_gain, w_query, w_key, w_value, w_out, bias, docs)

    return jax.shard_map(
        body,
        mesh=mesh,
        in_specs=(
            P("sp", "tp"),
            P(),
            P(None, "sp", "tp"),
            P(None, "sp", "tp"),
            P(None, "sp", "tp"),
            P(None, "tp", "sp"),
            P(None, "tp", None, None),
            P("sp"),
        ),
        out_specs=P("sp", "tp"),
        check_vma=False,
    )
```

```python
import functools

import jax
import jax.numpy as jnp
from jax import lax
from jax.experimental import pallas as pl
from jax.experimental.pallas import tpu as pltpu
from jax.sharding import PartitionSpec as P

HEAD_DIM = 64
WIN_ROWS = 8
WIN_COLS = 16
GRID_W = 32
EPS = 1e-06
MESH = pl.DeviceIdType.MESH
F32, BF16 = jnp.float32, jnp.bfloat16
K, V, Q, O = 0, 1, 2, 3


def kernel(n, nt, xs, layers, heads, tok_ref, gain_ref, wq_ref, wk_ref, wv_ref, wo_ref, bias_ref, doc_ref,
           out_ref, wbuf, obuf, xg, kv, part, s1, cs, s2, att, strip, dmask, docs,
           own_sem, w_send, w_recv, g_send, g_recv, h_send, h_recv, d_send, d_recv,
           r_send, r_recv, y_send, y_recv, b_send, b_recv):
    me, tp = lax.axis_index("sp"), lax.axis_index("tp")
    zs = n // xs
    toks, feat = tok_ref.shape
    reach = (WIN_ROWS // 2) * GRID_W
    after = reach - GRID_W
    wrows = wq_ref.shape[1]

    def pos_of(sp):
        z, x = sp // xs, sp % xs
        odd = x % 2
        return x * zs + z * (1 - odd) + (zs - 1 - z) * odd

    def sp_of(pos):
        x, z = pos // zs, pos % zs
        odd = x % 2
        return (z * (1 - odd) + (zs - 1 - z) * odd) * xs + x

    pos = pos_of(me)
    right, left = sp_of((pos + 1) % n), sp_of((pos + n - 1) % n)
    core = tp % 2
    mate = tp + 1 - 2 * core
    ymate = (tp + nt // 2) % nt
    has_prev = (me + n - 1) // n
    has_next = 1 - (me + 1) // n

    owns = []
    for l in range(layers):
        for c, ref in ((K, wk_ref), (V, wv_ref), (Q, wq_ref), (O, wo_ref)):
            dst = obuf.at[l, me] if c == O else wbuf.at[l, c, pl.ds(me * wrows, wrows)]
            copy = pltpu.make_async_copy(ref.at[l], dst, own_sem.at[l, c])
            copy.start()
            owns.append(copy)

    barrier = pltpu.get_barrier_semaphore()
    for peer in (left, right):
        pl.semaphore_signal(barrier, inc=1, device_id=(peer, tp), device_id_type=MESH)
    for d in range(1, nt):
        pl.semaphore_signal(barrier, inc=1, device_id=(me, (tp + d) % nt), device_id_type=MESH)

    @pl.when(me > 0)
    def _():
        pl.semaphore_signal(barrier, inc=1, device_id=(me - 1, tp), device_id_type=MESH)

    @pl.when(me < n - 1)
    def _():
        pl.semaphore_signal(barrier, inc=1, device_id=(me + 1, tp), device_id_type=MESH)

    pl.semaphore_wait(barrier, 1 + nt + has_prev + has_next)

    pending, halos = [], []

    def remote(src, dst, send, recv, device):
        return pltpu.make_async_remote_copy(src_ref=src, dst_ref=dst, send_sem=send, recv_sem=recv,
                                            device_id=device, device_id_type=MESH)

    half = n // 2
    RIGHTLAST, LEFTLAST = (K, V), (Q, O)

    def w_chunks(direction, step):
        if step < half:
            return (K, V, Q, O)
        if step == half:
            return RIGHTLAST if direction == 0 else LEFTLAST
        return ()

    def w_copy(direction, l, step, c):
        if direction == 0:
            origin, peer = sp_of((pos + n - (step - 1)) % n), right
        else:
            origin, peer = sp_of((pos + step - 1) % n), left
        ref = obuf.at[l, origin] if c == O else wbuf.at[l, c, pl.ds(origin * wrows, wrows)]
        return remote(ref, ref, w_send.at[direction, l, step - 1, c], w_recv.at[direction, l, step - 1, c],
                      (peer, tp))

    def w_arrive(direction, l, step, c):
        if direction == 0:
            origin = sp_of((pos + n - step) % n)
        else:
            origin = sp_of((pos + step) % n)
        ref = obuf.at[l, origin] if c == O else wbuf.at[l, c, pl.ds(origin * wrows, wrows)]
        remote(ref, ref, w_send.at[direction, l, step - 1, c], w_recv.at[direction, l, step - 1, c],
               (right if direction == 0 else left, tp)).wait_recv()

    def w_first(l, cs=range(4)):
        for c in cs:
            owns[l * 4 + c].wait()
            for direction in range(2):
                if c in w_chunks(direction, 1):
                    copy = w_copy(direction, l, 1, c)
                    copy.start()
                    pending.append(copy)

    def w_step(l, step, cs=range(4)):
        for c in cs:
            for direction in range(2):
                if c in w_chunks(direction, step):
                    w_arrive(direction, l, step, c)
                if c in w_chunks(direction, step + 1):
                    copy = w_copy(direction, l, step + 1, c)
                    copy.start()
                    pending.append(copy)

    tasks = []
    for l in range(layers):
        for step in range(1, half + 1):
            if step == half and l + 1 < layers:
                tasks += [(l, functools.partial(w_first, l + 1, (c,))) for c in range(4)]
            tasks += [(l, functools.partial(w_step, l, step, (c,))) for c in range(4)]

    def work(count, limit):
        while count > 0 and tasks and tasks[0][0] <= limit:
            tasks.pop(0)[1]()
            count -= 1

    w_first(0)
    gathers = []
    for d in range(1, nt):
        copy = remote(tok_ref, xg.at[0, tp], g_send.at[d - 1], g_recv.at[d - 1], (me, (tp + d) % nt))
        copy.start()
        gathers.append(copy)
    xg[0, tp] = tok_ref[...]

    def to_prev(src, dst, k):
        return remote(src, dst, h_send.at[0, k], h_recv.at[0, k], (jnp.maximum(me - 1, 0), tp))

    def to_next(src, dst, k):
        return remote(src, dst, h_send.at[1, k], h_recv.at[1, k], (jnp.minimum(me + 1, n - 1), tp))

    doc_prev = remote(doc_ref, docs.at[2], d_send.at[0], d_recv.at[0], ((me + n - 1) % n, tp))
    doc_next = remote(doc_ref, docs.at[0], d_send.at[1], d_recv.at[1], ((me + 1) % n, tp))

    @pl.when(me > 0)
    def _():
        doc_prev.start()

    @pl.when(me < n - 1)
    def _():
        doc_next.start()

    docs[1] = doc_ref[...]

    @pl.when(me == 0)
    def _():
        docs[0] = jnp.full_like(doc_ref, -1)
        for l in range(layers):
            kv[l, 0:reach] = jnp.zeros((reach, 2 * feat), BF16)

    @pl.when(me == n - 1)
    def _():
        docs[2] = jnp.full_like(doc_ref, -1)
        for l in range(layers):
            kv[l, reach + toks:reach + toks + after] = jnp.zeros((after, 2 * feat), BF16)

    work(4, 0)

    @pl.when(me > 0)
    def _():
        doc_next.wait_recv()

    @pl.when(me < n - 1)
    def _():
        doc_prev.wait_recv()

    seg = [docs[i].astype(F32) for i in range(3)]
    seg_row = jnp.concatenate(seg, axis=1)
    seg_col = jnp.transpose(jnp.broadcast_to(seg[1], (toks, toks)))
    lane = lax.broadcasted_iota(jnp.int32, (GRID_W, WIN_ROWS * GRID_W), 1) % GRID_W
    col = lax.broadcasted_iota(jnp.int32, (GRID_W, WIN_ROWS * GRID_W), 0)
    off = lane - col + WIN_COLS // 2
    inside = (off >= 0) & (off < WIN_COLS)
    rows = toks // GRID_W
    wide = WIN_ROWS * GRID_W
    for r in range(rows):
        keys = seg_row[:, r * GRID_W:(r + WIN_ROWS) * GRID_W]
        mine = seg_col[r * GRID_W:(r + 1) * GRID_W, 0:1]
        mask = jnp.where(inside & (keys == mine), 0.0, -1e30)
        dmask[r * GRID_W:(r + 1) * GRID_W] = pltpu.roll(mask, r * GRID_W, 1) if r else mask

    def fill_bias(l):
        for h in range(heads):
            row = jnp.broadcast_to(bias_ref[l * heads + h:l * heads + h + 1, :], (GRID_W, wide))
            base = pltpu.roll(row, wide - WIN_COLS // 2, 1, stride=1, stride_axis=0)
            for r in range(rows):
                cut = slice(r * GRID_W, (r + 1) * GRID_W)
                strip[l, h, cut] = (pltpu.roll(base, r * GRID_W, 1) if r else base) + dmask[cut]

    fill_bias(0)
    work(4, 0)
    for l in range(1, layers):
        fill_bias(l)
    for copy in gathers:
        copy.wait_recv()

    def head_norm(raw, scale):
        raw = raw.astype(BF16).astype(F32)
        sq = raw * raw
        outs = []
        for h in range(heads):
            cut = slice(h * HEAD_DIM, (h + 1) * HEAD_DIM)
            mean = jnp.sum(sq[:, cut], axis=-1, keepdims=True) * (1.0 / HEAD_DIM)
            outs.append(raw[:, cut] * (lax.rsqrt(mean + EPS) * scale))
        return jnp.concatenate(outs, axis=1).astype(BF16)

    for l in range(layers):
        x = [xg[l, q].astype(F32) for q in range(nt)]
        total = sum(jnp.sum(v * v, axis=-1, keepdims=True) for v in x)
        inv = lax.rsqrt(total * (1.0 / (nt * feat)) + EPS)
        normed = jnp.concatenate(
            [(x[q] * inv * gain_ref[l:l + 1, q * feat:(q + 1) * feat]).astype(BF16) for q in range(nt)], axis=1)
        while tasks and tasks[0][0] <= l:
            work(1, l)

        own = slice(reach, reach + toks)
        nxt = slice(reach + toks, reach + toks + after)
        hops = []
        for i, c in enumerate((K, V)):
            lanes = slice(i * feat, (i + 1) * feat)
            raw = jnp.dot(normed, wbuf[l, c], preferred_element_type=F32)
            kv[l, own, lanes] = head_norm(raw, 1.0) if c == K else raw.astype(BF16)
            up = to_next(kv.at[l, own, lanes], kv.at[l, 0:reach, lanes], 2 * l + i)
            down = to_prev(kv.at[l, reach:reach + after, lanes], kv.at[l, nxt, lanes], 2 * l + i)
            hops.append((up, down))

            @pl.when(me < n - 1)
            def _():
                up.start()

            @pl.when(me > 0)
            def _():
                down.start()

        halos += hops
        query = head_norm(jnp.dot(normed, wbuf[l, Q], preferred_element_type=F32), HEAD_DIM ** -0.5)
        work(4, l + 1)

        part_o, part_d = [], []
        for h in range(heads):
            cut = slice(h * HEAD_DIM, (h + 1) * HEAD_DIM)
            s = lax.dot_general(query[:, cut], kv[l, own, cut], (((1,), (1,)), ((), ())),
                                preferred_element_type=F32)
            p = jnp.exp(s + strip[l, h, :, reach:])
            part_d.append(jnp.sum(p, axis=-1, keepdims=True))
            part_o.append(jnp.dot(p.astype(BF16), kv[l, own, feat + h * HEAD_DIM:feat + (h + 1) * HEAD_DIM],
                                  preferred_element_type=F32))

        for up, down in hops:
            @pl.when(me > 0)
            def _():
                up.wait_recv()

            @pl.when(me < n - 1)
            def _():
                down.wait_recv()

        def halo(r, lanes):
            seam = r * GRID_W
            if not r:
                return kv[l, 0:reach, lanes]
            return jnp.concatenate([kv[l, reach + toks:reach + toks + seam, lanes], kv[l, seam:reach, lanes]], axis=0)

        for r in range(rows):
            keys, vals = halo(r, slice(0, feat)), halo(r, slice(feat, 2 * feat))
            rcut = slice(r * GRID_W, (r + 1) * GRID_W)
            for h in range(heads):
                cut = slice(h * HEAD_DIM, (h + 1) * HEAD_DIM)
                s = lax.dot_general(query[rcut, cut], keys[:, cut], (((1,), (1,)), ((), ())),
                                    preferred_element_type=F32)
                p = jnp.exp(s + strip[l, h, rcut, 0:reach])
                den = jnp.sum(p, axis=-1, keepdims=True) + part_d[h][rcut]
                o = jnp.dot(p.astype(BF16), vals[:, cut], preferred_element_type=F32) + part_o[h][rcut]
                att[rcut, cut] = (o / den).astype(BF16)

        a = att[...]
        per = feat // wo_ref.shape[2]

        def mix(q):
            return jnp.concatenate(
                [jnp.dot(a, obuf[l, q * per + i], preferred_element_type=F32) for i in range(per)], axis=1)

        s1c = []
        for j in range(2):
            part[l, j] = mix(1 - core + 2 * j).astype(BF16)
            copy = remote(part.at[l, j], s1.at[l, j], r_send.at[l, j], r_recv.at[l, j], (me, mate))
            copy.start()
            s1c.append(copy)
            pending.append(copy)
        mine = [mix(core + 2 * j) for j in range(2)]
        work(4, l + 1)
        last = l == layers - 1
        if not last:
            s2c = []
            for j in range(2):
                s1c[j].wait_recv()
                cs[l, j] = (mine[j] + s1[l, j].astype(F32)).astype(BF16)
                copy = remote(cs.at[l, j], s2.at[l, j], y_send.at[l, j], y_recv.at[l, j], (me, ymate))
                copy.start()
                s2c.append(copy)
                pending.append(copy)
            work(4, l + 1)
            s3c = []
            for j in range(2):
                s2c[j].wait_recv()
                slot = core + 2 * j
                xg[l + 1, slot] = (cs[l, j].astype(F32) + s2[l, j].astype(F32)).astype(BF16)
                copy = remote(xg.at[l + 1, slot], xg.at[l + 1, slot], b_send.at[l, j], b_recv.at[l, j], (me, mate))
                copy.start()
                s3c.append(copy)
                pending.append(copy)
            for j in range(2):
                s3c[j].wait_recv()
        else:
            y = tp // 2
            for j in range(2):
                s1c[j].wait_recv()
                cs[l, j] = (mine[j] + s1[l, j].astype(F32)).astype(BF16)
            copy = remote(cs.at[l, 1 - y], s2.at[l, 0], y_send.at[l, 0], y_recv.at[l, 0], (me, ymate))
            copy.start()
            pending.append(copy)
            copy.wait_recv()
            out_ref[...] = (cs[l, y].astype(F32) + s2[l, 0].astype(F32)).astype(BF16)

    for copy in gathers + pending:
        copy.wait_send()

    for up, down in halos:
        @pl.when(me < n - 1)
        def _():
            up.wait_send()

        @pl.when(me > 0)
        def _():
            down.wait_send()

    @pl.when(me > 0)
    def _():
        doc_prev.wait_send()

    @pl.when(me < n - 1)
    def _():
        doc_next.wait_send()


def solution(mesh):
    n, nt = mesh.shape["sp"], mesh.shape["tp"]
    try:
        xs = len({d.coords[0] for d in mesh.devices.flat})
    except AttributeError:
        xs = 2
    if n % xs or xs % 2:
        xs = 1

    def body(tokens, norm_gain, w_query, w_key, w_value, w_out, offset_bias, documents):
        layers, heads = offset_bias.shape[:2]
        toks, feat = tokens.shape
        model = nt * feat
        bias = jnp.pad(offset_bias, ((0, 0), (0, 0), (0, 0), (0, GRID_W - WIN_COLS)))
        bias = bias.reshape(layers * heads, WIN_ROWS * GRID_W)
        docs = documents.reshape(1, toks)
        reach = (WIN_ROWS // 2) * GRID_W
        dma = lambda *s: pltpu.SemaphoreType.DMA(s)
        vmem, hbm = pl.BlockSpec(memory_space=pltpu.VMEM), pl.BlockSpec(memory_space=pl.ANY)
        blocks = (layers, 2, toks, feat)
        return pl.pallas_call(
            functools.partial(kernel, n, nt, xs, layers, heads),
            out_shape=jax.ShapeDtypeStruct((toks, feat), BF16),
            in_specs=[vmem, vmem, hbm, hbm, hbm, hbm, vmem, vmem],
            out_specs=vmem,
            scratch_shapes=[
                pltpu.VMEM((layers, 3, model, feat), BF16),
                pltpu.VMEM((layers, n, feat, w_out.shape[2]), BF16),
                pltpu.VMEM((layers, nt, toks, feat), BF16),
                pltpu.VMEM((layers, 2 * reach - GRID_W + toks, 2 * feat), BF16),
                pltpu.VMEM(blocks, BF16),
                pltpu.VMEM(blocks, BF16),
                pltpu.VMEM(blocks, BF16),
                pltpu.VMEM(blocks, BF16),
                pltpu.VMEM((toks, feat), BF16),
                pltpu.VMEM((layers, heads, toks, WIN_ROWS * GRID_W), F32),
                pltpu.VMEM((toks, WIN_ROWS * GRID_W), F32),
                pltpu.VMEM((3, 1, toks), jnp.int32),
                dma(layers, 4),
                dma(2, layers, n // 2, 4), dma(2, layers, n // 2, 4),
                dma(nt - 1), dma(nt - 1),
                dma(2, 2 * layers), dma(2, 2 * layers),
                dma(2), dma(2),
                dma(layers, 2), dma(layers, 2),
                dma(layers, 2), dma(layers, 2),
                dma(layers, 2), dma(layers, 2),
            ],
            compiler_params=pltpu.CompilerParams(
                collective_id=0, has_side_effects=True, vmem_limit_bytes=48 * 1024 * 1024
            ),
        )(tokens, norm_gain, w_query, w_key, w_value, w_out, bias, docs)

    return jax.shard_map(
        body,
        mesh=mesh,
        in_specs=(
            P("sp", "tp"),
            P(),
            P(None, "sp", "tp"),
            P(None, "sp", "tp"),
            P(None, "sp", "tp"),
            P(None, "tp", "sp"),
            P(None, "tp", None, None),
            P("sp"),
        ),
        out_specs=P("sp", "tp"),
        check_vma=False,
    )
```
